32 devices in a mesh: sp: 8 (over z, y), tp: 4 (over x, core).
Axes of the slice: x: 2, y: 2, z: 4, core: 2. Of those that a mesh axis runs over, the one named last changes fastest.
Arguments:
- glu_value: bfloat16 [4096, 2048], P('sp', 'tp'), may hold values from -640 to 640
- glu_gate: bfloat16 [4096, 2048], P('sp', 'tp'), may hold values from -9 to 9
- conv_kernel: float32 [31, 2048], P(None, 'tp'), may hold values from -1 to 1
- norm_gain: float32 [2048], P('tp'), may hold values from 0.1 to 1.9
- mix_weight: bfloat16 [2048, 2048], P('tp'), may hold values from -0.125 to 0.125
- residual: bfloat16 [4096, 2048], P(('sp', 'tp')), may hold values from -6 to 6
- resid_gain: float32 [2048], replicated, may hold values from 0.1 to 1.9
- expert_ids: int32 [4096, 2], P(('sp', 'tp')), may hold values from 0 to 7, all different within a row; in each aligned block of 128 rows (0 to 127, 128 to 255, ...) at most 64 rows name the same one
- route_weight: float32 [4096, 2], P(('sp', 'tp')), may hold values from 0.05 to 0.5
- w_gate: bfloat16 [8, 2048, 2048], P('sp', None, 'tp'), may hold values from -0.5 to 0.5
- w_up: bfloat16 [8, 2048, 2048], P('sp', None, 'tp'), may hold values from -0.5 to 0.5
- w_down: bfloat16 [8, 2048, 2048], P('sp', 'tp'), may hold values from -0.03125 to 0.03125
- out_gain: float32 [2048], replicated, may hold values from 0.1 to 1.9
Outputs:
- blended: bfloat16 [4096, 2048], P(('sp', 'tp'))
The draws below stay inside these ranges and needn't reach their ends.
Inputs may be any that keep to these rules, and one draw needn't show every extreme that they name: `expert_ids`: in each aligned block of 128 rows (the rows of one device) no expert is named by more than 64 rows, a bound that some block reaches.
All inputs are finite; a program needn't handle non-finite values.
Results may differ from the reference program's by a relative error of at most 0.015.
Values may be sent and summed in bfloat16 or wider, within the bound.
A program may use at most 128 MiB of HBM per device.

```python
import math
from functools import partial
import jax
import jax.numpy as jnp
import numpy as np
from jax import lax

D = 2048
DC = 2048
FFE = 2048
KERNEL = 31
TOPK = 2
TOKENS = 4096
BLOCK = 128
EXPERTS = 8
CAP = 64
N_SP = 8
N_TP = 4


def draw_glu_value(key, part):
    key_rough, key_base = jax.random.split(key, 2)
    ramp = 10.0 ** (jnp.arange(DC, dtype=jnp.float32) / DC)
    rough = jax.random.uniform(key_rough, (DC,), jnp.float32, 0.5, 1.5)
    base = jnp.clip(jax.random.normal(key_base, (TOKENS, DC), jnp.float32), -6.0, 6.0)
    return (0.5 * ramp * rough * base).astype(jnp.bfloat16)


def shard_levels(own_key, extent, cuts, least, high):
    level = 1.0
    for dim, shards_of in cuts:
        steps = jax.random.uniform(jax.random.fold_in(jax.random.fold_in(own_key, 6), dim), (shards_of,), jnp.float32, least / len(cuts), high / len(cuts))
        level = level * jnp.repeat(jnp.exp(steps), extent[dim] // shards_of).reshape((-1,) + (1,) * (len(extent) - 1 - dim))
    return level


def routed_block(rng, own, number, rows, number_of, top, bound, skew):
    order = jax.random.permutation(rng, number_of)
    crowded, usual = portions_of(number_of, rows * top, bound, skew, True), portions_of(number_of, rows * top, bound, skew, False)
    places = jnp.arange(number_of)

    def named(tallies, turn):
        used = int((tallies > 0).sum())
        fixed = max(1, used // 4)
        moved = fixed + (places - fixed + turn * (used - fixed)) % max(1, number_of - fixed)
        return jnp.zeros((number_of,), jnp.int32).at[order[jnp.where(places < fixed, places, moved)]].set(jnp.asarray(tallies, jnp.int32))

    tallies = jnp.where(number % 4 == 0, named(crowded, number // 4), named(usual, number - number // 4 - 1))
    mixed = jax.random.permutation(jax.random.fold_in(own, 3), number_of)
    giver, sink = mixed[0:number_of // 2 * 2:2], mixed[1:number_of // 2 * 2:2]
    margin = jnp.minimum(tallies[giver] - 1, bound - tallies[sink]) // 2
    margin = jnp.where((giver == order[0]) | (sink == order[0]) | (tallies[sink] == 0), 0, jnp.maximum(margin, 0))
    moved = jax.random.randint(jax.random.fold_in(own, 4), (number_of // 2,), 0, 1 << 20) % (margin + 1)
    tallies = tallies.at[giver].add(-moved).at[sink].add(moved)
    items = jnp.searchsorted(jnp.cumsum(tallies), jnp.arange(rows * top), side="right").astype(jnp.int32)
    grid = items.reshape(top, rows).T
    grid = grid[jax.random.permutation(jax.random.fold_in(own, 1), rows)]
    turn = jax.random.randint(jax.random.fold_in(own, 2), (rows, 1), 0, top)
    return jnp.take_along_axis(grid, (jnp.arange(top)[None, :] + turn) % top, axis=1)


def portions_of(number_of, total, reach, skew, full):
    loads = [(1 << 20) // math.isqrt(rank ** skew) + 1 for rank in range(1, number_of + 1)]
    largest = reach if full else min(reach, max(-(-total // number_of), total * loads[0] // sum(loads)))
    least = 1 if total - largest >= number_of - 1 else 0
    holding, spare = [largest] + [least] * (number_of - 1), total - largest - least * (number_of - 1)
    while spare > 0:
        candidates = [i for i in range(1, number_of) if holding[i] < largest] or [i for i in range(1, number_of) if holding[i] < reach]
        mass, budget = sum([loads[i] for i in candidates]), spare
        for i in candidates:
            addition = min(reach - holding[i], max(1, budget * loads[i] // mass), spare)
            holding[i] = holding[i] + addition
            spare = spare - addition
    return np.array(holding)


def noise(stream_key, dims, scale, limit, cuts=(), kind=jnp.bfloat16):
    factor_of = shard_levels(stream_key, dims, cuts, -0.22, 0.18) if cuts else 1.0
    values = jax.random.normal(stream_key, dims, jnp.float32) * scale * factor_of
    return jnp.minimum(jnp.maximum(values, -limit), limit).astype(kind)


def setup_inputs(seed: int = 0) -> dict:
    splits = jax.random.split(jax.random.key(seed), 14)
    glu_value = draw_glu_value(jax.random.fold_in(splits[13], 71), 0)
    glu_gate = noise(splits[1], (TOKENS, DC), 1.5, 9.0, ((0, 8), (1, 4)))
    conv_kernel = noise(splits[2], (KERNEL, DC), KERNEL ** -0.5, 1.0, ((1, 4),), jnp.float32)
    norm_gain = jnp.clip(1.0 + 0.18 * jax.random.normal(splits[3], (DC,), jnp.float32), 0.1, 1.9)
    mix_weight = noise(splits[4], (DC, D), DC ** -0.5, 0.125, ((0, 4),))
    residual = noise(splits[5], (TOKENS, D), 1.0, 6.0, ((0, 32),))
    resid_gain = jnp.clip(1.0 + 0.18 * jax.random.normal(splits[6], (D,), jnp.float32), 0.1, 1.9)
    expert_ids_keys = jax.random.split(jax.random.fold_in(splits[7], 1), TOKENS // BLOCK)
    expert_ids_turns = jax.random.permutation(jax.random.fold_in(splits[7], 3), TOKENS // BLOCK)
    expert_ids = jax.vmap(lambda own, number: routed_block(jax.random.fold_in(splits[7], 2), own, number, BLOCK, EXPERTS, TOPK, CAP, 2))(expert_ids_keys, expert_ids_turns).reshape((TOKENS, TOPK))
    route_weight = jnp.clip(jnp.exp(math.log(0.5) - 2.3025851 * jax.random.uniform(splits[8], (TOKENS, TOPK), jnp.float32) ** shard_levels(splits[8], (TOKENS, TOPK), ((0, 32),), -0.2, 0.2)), 0.05, 0.5)
    w_gate = noise(splits[9], (EXPERTS, D, FFE), (D // 16) ** -0.5, 0.5, ((0, 8), (2, 4)))
    w_up = noise(splits[10], (EXPERTS, D, FFE), (D // 16) ** -0.5, 0.5, ((0, 8), (2, 4)))
    w_down = noise(splits[11], (EXPERTS, FFE, D), (16 * FFE) ** -0.5, 0.03125, ((0, 8), (1, 4)))
    out_gain = jnp.clip(1.0 + 0.18 * jax.random.normal(splits[12], (D,), jnp.float32), 0.1, 1.9)
    return {"glu_value": glu_value, "glu_gate": glu_gate, "conv_kernel": conv_kernel, "norm_gain": norm_gain, "mix_weight": mix_weight, "residual": residual, "resid_gain": resid_gain, "expert_ids": expert_ids, "route_weight": route_weight, "w_gate": w_gate, "w_up": w_up, "w_down": w_down, "out_gain": out_gain}


EPSILON = 1e-05
LIMIT = 7.0
SLOPE = 1.702

def normalize(values, gain_vector):
    centre = lax.optimization_barrier(jnp.mean(values, axis=-1, keepdims=True))
    spread = lax.optimization_barrier(jnp.mean(jnp.square(values - centre), axis=-1, keepdims=True))
    return (values - centre) * lax.rsqrt(spread + EPSILON) * gain_vector

def slot_layout(route_ids, experts, capacity):
    row_count, top_count = route_ids.shape
    flat_ids = route_ids.reshape(row_count * top_count).astype(jnp.int32)
    onehot = (flat_ids[:, None] == jnp.arange(experts, dtype=jnp.int32)[None, :]).astype(jnp.int32)
    before = jnp.cumsum(onehot, axis=0) - onehot
    slot_rank = lax.optimization_barrier(jnp.sum(before * onehot, axis=1)).astype(jnp.int32)
    position = (flat_ids * capacity + slot_rank).astype(jnp.int32)
    owners = (jnp.arange(row_count * top_count, dtype=jnp.int32) // top_count).astype(jnp.int32)
    slot_table = jnp.full((experts * capacity,), row_count, jnp.int32).at[position].set(owners)
    return (slot_table, position.reshape(row_count, top_count))

def run_expert(operands):
    tokens, gate_matrix, up_matrix, down_matrix = operands
    tokens_wide = tokens.astype(jnp.float32)
    gate_pre = jnp.dot(tokens_wide, gate_matrix.astype(jnp.float32), preferred_element_type=jnp.float32)
    up_pre = jnp.dot(tokens_wide, up_matrix.astype(jnp.float32), preferred_element_type=jnp.float32)
    gated = jnp.minimum(gate_pre, LIMIT)
    upper = jnp.clip(up_pre, -LIMIT, LIMIT)
    activity = ((upper + 1.0) * gated * jax.nn.sigmoid(SLOPE * gated)).astype(jnp.bfloat16)
    quarter = FFE // N_TP
    pieces = activity.reshape(-1, N_TP, quarter).astype(jnp.float32)
    downs = down_matrix.reshape(N_TP, quarter, D).astype(jnp.float32)
    partials = jnp.einsum('rqf,qfd->qrd', pieces, downs).astype(jnp.bfloat16)
    partials = lax.optimization_barrier(partials)
    return lax.optimization_barrier(jnp.sum(partials.astype(jnp.float32), axis=0)).astype(jnp.bfloat16)

def reference(glu_value, glu_gate, conv_kernel, norm_gain, mix_weight, residual, resid_gain, expert_ids, route_weight, w_gate, w_up, w_down, out_gain):
    gated_in = (glu_value.astype(jnp.float32) * jax.nn.sigmoid(glu_gate.astype(jnp.float32))).astype(jnp.bfloat16)
    extended = jnp.pad(gated_in.astype(jnp.float32), ((KERNEL - 1, 0), (0, 0)))
    convolved = jnp.zeros((TOKENS, DC), jnp.float32)
    for offset in range(KERNEL):
        convolved = convolved + conv_kernel[offset] * extended[offset:offset + TOKENS]
    centre = lax.optimization_barrier(jnp.mean(convolved, axis=1, keepdims=True))
    spread = lax.optimization_barrier(jnp.mean(jnp.square(convolved), axis=1, keepdims=True)) - centre * centre
    normed = (convolved - centre) * lax.rsqrt(spread + EPSILON) * norm_gain
    mix_in = jax.nn.silu(normed).astype(jnp.bfloat16)
    mixed_rows = jnp.dot(mix_in, mix_weight, preferred_element_type=jnp.float32)
    hidden = normalize(residual.astype(jnp.float32) + mixed_rows, resid_gain).astype(jnp.bfloat16)
    block_count = N_SP * N_TP
    block_ids = expert_ids.reshape(block_count, BLOCK, TOPK)
    tables, positions = jax.vmap(partial(slot_layout, experts=EXPERTS, capacity=CAP))(block_ids)
    hidden_blocks = hidden.reshape(block_count, BLOCK, D)
    padded = jnp.concatenate([hidden_blocks, jnp.zeros((block_count, 1, D), jnp.bfloat16)], axis=1)
    slot_rows = jax.vmap(partial(jnp.take, axis=0))(padded, tables)
    expert_major = slot_rows.reshape(block_count, EXPERTS, CAP, D).transpose(1, 0, 2, 3)
    expert_major = expert_major.reshape(EXPERTS, block_count * CAP, D)
    outputs = lax.map(run_expert, (expert_major, w_gate, w_up, w_down))
    block_major = outputs.reshape(EXPERTS, block_count, CAP, D).transpose(1, 0, 2, 3)
    block_major = block_major.reshape(block_count, EXPERTS * CAP, D)
    picked = jax.vmap(partial(jnp.take, axis=0))(block_major, positions.reshape(block_count, BLOCK * TOPK))
    picked = picked.reshape(TOKENS, TOPK, D)
    routed_sum = jnp.einsum('tk,tkd->td', route_weight.astype(jnp.float32), picked.astype(jnp.float32))
    return normalize(hidden.astype(jnp.float32) + routed_sum, out_gain).astype(jnp.bfloat16)
```

```python
import functools

import jax
import jax.numpy as jnp
from jax import lax
from jax.experimental import pallas as pl
from jax.experimental.pallas import tpu as pltpu
from jax.sharding import PartitionSpec as P


DC = 2048


EPSILON = 1e-05
LIMIT = 7.0
SLOPE = 1.702


def shifted(block, axis, distance):
    devices = range(lax.axis_size(axis))
    route = [(i - distance, i) for i in devices if i - distance in devices]
    return lax.ppermute(block, axis, route)


def normalize(values, gain_vector):
    centre = jnp.mean(values, axis=-1, keepdims=True)
    spread = jnp.mean(jnp.square(values - centre), axis=-1, keepdims=True)
    return (values - centre) * lax.rsqrt(spread + EPSILON) * gain_vector


def swapped(block, stride):
    route = [(i, i ^ stride) for i in range(lax.axis_size("tp"))]
    return lax.ppermute(block, "tp", route)


def slot_layout(route_ids, experts, capacity):
    row_count, top_count = route_ids.shape
    flat_ids = route_ids.reshape(row_count * top_count)
    onehot = (flat_ids[:, None] == jnp.arange(experts, dtype=jnp.int32)[None, :]).astype(jnp.int32)
    before = jnp.cumsum(onehot, axis=0) - onehot
    slot_rank = jnp.sum(before * onehot, axis=1)
    position = flat_ids * capacity + slot_rank
    return position.reshape(row_count, top_count)


def expert_activity(tokens, gate_matrix, up_matrix):
    gate_pre = jnp.dot(tokens, gate_matrix, preferred_element_type=jnp.float32)
    up_pre = jnp.dot(tokens, up_matrix, preferred_element_type=jnp.float32)
    gated = jnp.minimum(gate_pre, LIMIT)
    upper = jnp.clip(up_pre, -LIMIT, LIMIT)
    return ((upper + 1.0) * gated * jax.nn.sigmoid(SLOPE * gated)).astype(jnp.bfloat16)


MESH = pl.DeviceIdType.MESH


def exchange_kernel(count, forward, sent, out, local_sem, send_sem, recv_sem, pass_sem, land_sem):
    me = lax.axis_index("sp")
    place = lax.axis_index("tp")
    partner = place + 1 - 2 * lax.rem(place, 2)
    mine = out.at[0] if forward else out

    barrier = pltpu.get_barrier_semaphore()
    for step in range(1, count):
        peer = lax.rem(me + step, count)
        pl.semaphore_signal(barrier, inc=1, device_id={"sp": peer}, device_id_type=MESH)
    if forward:
        pl.semaphore_signal(barrier, inc=1, device_id={"tp": partner}, device_id_type=MESH)
    pl.semaphore_wait(barrier, count - 1 + int(forward))

    copies = []
    for step in range(1, count):
        peer = lax.rem(me + step, count)
        copy = pltpu.make_async_remote_copy(
            src_ref=sent.at[peer],
            dst_ref=mine.at[me],
            send_sem=send_sem.at[step],
            recv_sem=recv_sem.at[step],
            device_id={"sp": peer},
            device_id_type=MESH,
        )
        copy.start()
        copies.append(copy)
    kept = pltpu.make_async_copy(sent.at[me], mine.at[me], local_sem)
    kept.start()

    def passed(block, source, step):
        return pltpu.make_async_remote_copy(
            src_ref=block,
            dst_ref=out.at[1, source],
            send_sem=pass_sem.at[step],
            recv_sem=land_sem.at[step],
            device_id={"tp": partner},
            device_id_type=MESH,
        )

    passes = []
    if forward:
        passes.append(passed(sent.at[me], me, 0))
        passes[0].start()
    order = sorted(range(1, count), key=lambda step: min(step, count - step))
    for step in order:
        source = lax.rem(me + count - step, count)
        pltpu.make_async_remote_copy(
            src_ref=sent.at[source],
            dst_ref=mine.at[source],
            send_sem=send_sem.at[step],
            recv_sem=recv_sem.at[step],
            device_id={"sp": source},
            device_id_type=MESH,
        ).wait_recv()
        if forward:
            one = passed(mine.at[source], source, step)
            one.start()
            passes.append(one)
    kept.wait()
    for copy in copies:
        copy.wait_send()
    for one in passes:
        one.wait()


def exchange(blocks, forward, number):
    count = blocks.shape[0]
    shape = ((2,) if forward else ()) + blocks.shape
    size = blocks.size * 2
    return pl.pallas_call(
        functools.partial(exchange_kernel, count, forward),
        out_shape=jax.ShapeDtypeStruct(shape, blocks.dtype),
        in_specs=[pl.BlockSpec(memory_space=pl.ANY)],
        out_specs=pl.BlockSpec(memory_space=pl.ANY),
        scratch_shapes=[
            pltpu.SemaphoreType.DMA,
            pltpu.SemaphoreType.DMA((count,)),
            pltpu.SemaphoreType.DMA((count,)),
            pltpu.SemaphoreType.DMA((count,)),
            pltpu.SemaphoreType.DMA((count,)),
        ],
        compiler_params=pltpu.CompilerParams(collective_id=number, has_side_effects=True),
        cost_estimate=pl.CostEstimate(flops=0, bytes_accessed=size * 40, transcendentals=0),
    )(blocks)


def shards(
    glu_value,
    glu_gate,
    conv_kernel,
    norm_gain,
    mix_weight,
    residual,
    resid_gain,
    expert_ids,
    route_weight,
    w_gate,
    w_up,
    w_down,
    out_gain,
):
    gate_local, up_local, down_local = w_gate[0], w_up[0], w_down[0]
    depth = gate_local.shape[0]
    first, second = depth // 2, depth * 3 // 4
    left = down_local.shape[1] * 3 // 8
    gate_far = jnp.concatenate(
        [
            swapped(gate_local[:first], 2),
            swapped(gate_local[first:second], 2),
            swapped(gate_local[second:], 2),
        ],
        axis=0,
    )
    up_far = swapped(up_local, 2)
    down_far = (swapped(down_local[:, :left], 2), swapped(down_local[:, left:], 2))
    gated_in = (
        glu_value.astype(jnp.float32) * jax.nn.sigmoid(glu_gate.astype(jnp.float32))
    ).astype(jnp.bfloat16)
    reach_back = conv_kernel.shape[0] - 1
    length = gated_in.shape[0]
    before_rows = shifted(gated_in[length - reach_back :], "sp", 1)
    extended = jnp.concatenate([before_rows, gated_in], axis=0).astype(jnp.float32)
    convolved = jnp.zeros(gated_in.shape, jnp.float32)
    for offset in range(reach_back + 1):
        convolved = convolved + conv_kernel[offset] * extended[offset : offset + length]
    channel_sum, squares = lax.psum(
        (jnp.sum(convolved, axis=1), jnp.sum(convolved * convolved, axis=1)), "tp"
    )
    centre = channel_sum / DC
    spread = squares / DC - centre * centre
    normed = (convolved - centre[:, None]) * lax.rsqrt(spread[:, None] + EPSILON) * norm_gain
    mix_in = jax.nn.silu(normed).astype(jnp.bfloat16)
    tp_count = lax.axis_size("tp")
    place = lax.axis_index("tp")
    own_count = length // tp_count
    width = residual.shape[1]
    products = jnp.dot(mix_in, mix_weight, preferred_element_type=jnp.float32)
    products = products.astype(jnp.bfloat16).reshape(tp_count // 2, 2, own_count, width)
    near = place % 2
    far = place // 2
    kept = lax.dynamic_index_in_dim(products, near, 1, False)
    given = lax.dynamic_index_in_dim(products, 1 - near, 1, False)
    pair_sum = kept.astype(jnp.float32) + swapped(given, 1).astype(jnp.float32)
    pair_kept = lax.dynamic_index_in_dim(pair_sum, far, 0, False)
    pair_given = lax.dynamic_index_in_dim(pair_sum, 1 - far, 0, False).astype(jnp.bfloat16)
    mixed_rows = pair_kept + swapped(pair_given, 2).astype(jnp.float32)
    hidden = normalize(residual.astype(jnp.float32) + mixed_rows, resid_gain).astype(jnp.bfloat16)
    experts = lax.axis_size("sp")
    top_count = expert_ids.shape[1]
    capacity = 2 * own_count * top_count // experts
    positions = slot_layout(expert_ids, experts, capacity)
    slots = jnp.arange(experts * capacity, dtype=jnp.int32)
    chosen = (positions[:, :, None] == slots).astype(jnp.float32)
    pick = jnp.sum(chosen, axis=1).astype(jnp.bfloat16)
    weights = jnp.sum(chosen * route_weight[:, :, None], axis=1)
    weights_high = weights.astype(jnp.bfloat16)
    weights_low = (weights - weights_high.astype(jnp.float32)).astype(jnp.bfloat16)
    dispatched = lax.dot_general(
        pick, hidden, (((0,), (0,)), ((), ())), preferred_element_type=jnp.float32
    ).astype(jnp.bfloat16)
    dispatched = dispatched.reshape(experts, capacity, width)
    arrived = exchange(dispatched, True, 0)
    rows = arrived.reshape(2 * experts * capacity, width)
    act_local = expert_activity(rows, gate_local, up_local)
    act_far = expert_activity(rows, gate_far, up_far)
    sums = []
    for part in range(2):
        columns = slice(0, left) if part == 0 else slice(left, width)
        share = down_far[part].shape[1]
        out = jnp.dot(
            act_local, down_local[:, columns], preferred_element_type=jnp.float32
        ) + jnp.dot(act_far, down_far[part], preferred_element_type=jnp.float32)
        out = out.astype(jnp.bfloat16).reshape(2, experts * capacity, share)
        given_out = swapped(out[1], 1)
        expert_out = (out[0].astype(jnp.float32) + given_out.astype(jnp.float32)).astype(jnp.bfloat16)
        returned = exchange(expert_out.reshape(experts, capacity, share), False, 1 + part)
        returned = returned.reshape(experts * capacity, share)
        sums.append(
            jnp.dot(weights_high, returned, preferred_element_type=jnp.float32)
            + jnp.dot(weights_low, returned, preferred_element_type=jnp.float32)
        )
    routed_sum = jnp.concatenate(sums, axis=1)
    return normalize(hidden.astype(jnp.float32) + routed_sum, out_gain).astype(jnp.bfloat16)


def solution(mesh):
    in_specs = (
        P("sp", "tp"),
        P("sp", "tp"),
        P(None, "tp"),
        P("tp"),
        P("tp", None),
        P(("sp", "tp"), None),
        P(),
        P(("sp", "tp"), None),
        P(("sp", "tp"), None),
        P("sp", None, "tp"),
        P("sp", None, "tp"),
        P("sp", "tp", None),
        P(),
    )
    out_specs = P(("sp", "tp"), None)

    return jax.shard_map(shards, mesh=mesh, in_specs=in_specs, out_specs=out_specs, check_vma=False)
```
